512 devices in a mesh: ep: 32 (over z, core), tp: 16 (over y, x).
Axes of the slice: x: 4, y: 4, z: 16, core: 2. Of those that a mesh axis runs over, the one named last changes fastest.
Arguments:
- tokens: bfloat16 [1024, 2048], P('ep', 'tp'), may hold values from -200 to 200
- routing: int32 [1024, 4], P('ep'), may hold values from 0 to 63, all different within a row; in each aligned block of 32 rows (0 to 31, 32 to 63, ...) at most 8 rows name the same one
- gate_weights: float32 [1024, 4], P('ep'), may hold values from 0.05 to 1
- norm_gain: float32 [2048], replicated, may hold values from 0.1 to 1.9
- w_gate: bfloat16 [64, 2048, 2048], P('ep', None, 'tp'), may hold values from -0.33007812 to 0.33007812
- w_up: bfloat16 [64, 2048, 2048], P('ep', None, 'tp'), may hold values from -0.33007812 to 0.33007812
- w_down: bfloat16 [64, 2048, 2048], P('ep', 'tp'), may hold values from -0.026489258 to 0.026489258
Outputs:
- mixed: bfloat16 [1024, 2048], P('ep', 'tp')
The draws below stay inside these ranges and needn't reach their ends.
Inputs may be any that keep to these rules, and one draw needn't show every extreme that they name: `routing`: each token names 4 different experts. Among the 32 tokens of one index of ep no expert is named more than 8 times, a bound that some block reaches.
All inputs are finite; a program needn't handle non-finite values.
Results may differ from the reference program's by a relative error of at most 0.015.
Values may be sent and summed in bfloat16 or wider, within the bound.
A program may use at most 128 MiB of HBM per device.

```python
import math
import jax
import jax.numpy as jnp
import numpy as np
from jax import lax

D = 2048
FF = 2048
TOP = 4
EXP_DEV = 2
TOK_DEV = 32
CAP = 8
EXPERTS = 64
TOKENS = 1024
N_EP = 32
N_TP = 16


def draw_tokens(key, part):
    base_key, scale_key, row_key, mean_key = jax.random.split(key, 4)
    values = jax.random.normal(base_key, (TOKENS, D), jnp.float32)
    values = jnp.clip(values, -6.0, 6.0)
    column_scale = jnp.exp(jax.random.uniform(scale_key, (D // 16,), jnp.float32, jnp.log(0.3), jnp.log(3.0)))
    values = values * jnp.repeat(column_scale, 16)[None, :]
    return values.astype(jnp.bfloat16)


def block_levels(stream_key, dims, cuts, smallest, top_value):
    loudness = 1.0
    for axis_at, shards_of in cuts:
        draws = jax.random.uniform(jax.random.fold_in(jax.random.fold_in(stream_key, 6), axis_at), (shards_of,), jnp.float32, smallest / len(cuts), top_value / len(cuts))
        loudness = loudness * jnp.repeat(jnp.exp(draws), dims[axis_at] // shards_of).reshape((-1,) + (1,) * (len(dims) - 1 - axis_at))
    return loudness


def routed_block(key, own, number, rows, count, top, most, skew):
    order = jax.random.permutation(key, count)
    crowded, common = load_shares(count, rows * top, most, skew, True), load_shares(count, rows * top, most, skew, False)
    places = jnp.arange(count)

    def named(lengths, rotation):
        used = int((lengths > 0).sum())
        fixed = max(1, used // 4)
        moved = fixed + (places - fixed + rotation * (used - fixed)) % max(1, count - fixed)
        return jnp.zeros((count,), jnp.int32).at[order[jnp.where(places < fixed, places, moved)]].set(jnp.asarray(lengths, jnp.int32))

    lengths = jnp.where(number % 4 == 0, named(crowded, number // 4), named(common, number - number // 4 - 1))
    mixed = jax.random.permutation(jax.random.fold_in(own, 3), count)
    giver, taker = mixed[0:count // 2 * 2:2], mixed[1:count // 2 * 2:2]
    room = jnp.minimum(lengths[giver] - 1, most - lengths[taker]) // 2
    room = jnp.where((giver == order[0]) | (taker == order[0]) | (lengths[taker] == 0), 0, jnp.maximum(room, 0))
    moved = jax.random.randint(jax.random.fold_in(own, 4), (count // 2,), 0, 1 << 20) % (room + 1)
    lengths = lengths.at[giver].add(-moved).at[taker].add(moved)
    members = jnp.searchsorted(jnp.cumsum(lengths), jnp.arange(rows * top), side="right").astype(jnp.int32)
    listing = members.reshape(top, rows).T
    listing = listing[jax.random.permutation(jax.random.fold_in(own, 1), rows)]
    rotation = jax.random.randint(jax.random.fold_in(own, 2), (rows, 1), 0, top)
    return jnp.take_along_axis(listing, (jnp.arange(top)[None, :] + rotation) % top, axis=1)


def load_shares(amount, total, most, slope, full):
    weights = [(1 << 20) // math.isqrt(grade ** slope) + 1 for grade in range(1, amount + 1)]
    largest = most if full else min(most, max(-(-total // amount), total * weights[0] // sum(weights)))
    least = 1 if total - largest >= amount - 1 else 0
    counts, rest = [largest] + [least] * (amount - 1), total - largest - least * (amount - 1)
    while rest > 0:
        free = [i for i in range(1, amount) if counts[i] < largest] or [i for i in range(1, amount) if counts[i] < most]
        whole, left = sum([weights[i] for i in free]), rest
        for i in free:
            more = min(most - counts[i], max(1, left * weights[i] // whole), rest)
            counts[i] = counts[i] + more
            rest = rest - more
    return np.array(counts)


def scatter_about(key, shape, deviation, reach, pieces=(), held_as=jnp.bfloat16):
    drawn = deviation * jax.random.normal(key, shape, jnp.float32)
    if pieces:
        drawn = drawn * block_levels(key, shape, pieces, -0.22, 0.18)
    return jnp.clip(drawn, -reach, reach).astype(held_as)


def setup_inputs(seed: int = 0) -> dict:
    keys = jax.random.split(jax.random.key(seed), 8)
    tokens = draw_tokens(jax.random.fold_in(keys[7], 71), 0)
    routing_keys = jax.random.split(jax.random.fold_in(keys[1], 1), TOKENS // TOK_DEV)
    routing_turns = jax.random.permutation(jax.random.fold_in(keys[1], 3), TOKENS // TOK_DEV)
    routing = jax.vmap(lambda own, number: routed_block(jax.random.fold_in(keys[1], 2), own, number, TOK_DEV, EXP_DEV * N_EP, TOP, CAP, 2))(routing_keys, routing_turns).reshape((TOKENS, TOP))
    gate_weights = jnp.clip(jnp.exp(math.log(1.0) - 2.9957323 * jax.random.uniform(keys[2], (TOKENS, TOP), jnp.float32) ** block_levels(keys[2], (TOKENS, TOP), ((0, 32),), -0.2, 0.2)), 0.05, 1.0)
    norm_gain = jnp.clip(1.0 + 0.18 * jax.random.normal(keys[3], (D,), jnp.float32), 0.1, 1.9)
    w_gate = scatter_about(keys[4], (EXPERTS, D, FF), (2.5 * D ** -0.5), 0.33007812, ((0, 32), (2, 16)))
    w_up = scatter_about(keys[5], (EXPERTS, D, FF), (2.5 * D ** -0.5), 0.33007812, ((0, 32), (2, 16)))
    w_down = scatter_about(keys[6], (EXPERTS, FF, D), (0.2 * FF ** -0.5), 0.026489258, ((0, 32), (1, 16)))
    return dict(tokens=tokens, routing=routing, gate_weights=gate_weights, norm_gain=norm_gain, w_gate=w_gate, w_up=w_up, w_down=w_down)


norm_eps = 1e-06
clamp_limit = 7.0
swish_alpha = 1.702

def expert_apply(inputs):
    rows, gate_mat, up_mat, down_mat = inputs
    pre_gate = jnp.dot(rows, gate_mat, preferred_element_type=jnp.float32)
    pre_up = jnp.dot(rows, up_mat, preferred_element_type=jnp.float32)
    clamped = jnp.minimum(pre_gate, clamp_limit)
    upper = jnp.clip(pre_up, -clamp_limit, clamp_limit)
    hidden = (clamped * jax.nn.sigmoid(swish_alpha * clamped) * (upper + 1.0)).astype(jnp.bfloat16)
    block_width = FF // N_TP
    hidden_blocks = hidden.reshape(hidden.shape[0], N_TP, block_width).astype(jnp.float32)
    down_blocks = down_mat.reshape(N_TP, block_width, D).astype(jnp.float32)
    partial_value = jnp.einsum('rnf,nfd->nrd', hidden_blocks, down_blocks)
    rounded = partial_value.astype(jnp.bfloat16).astype(jnp.float32)
    return lax.optimization_barrier(jnp.sum(rounded, axis=0)).astype(jnp.bfloat16)

def reference(tokens, routing, gate_weights, norm_gain, w_gate, w_up, w_down):
    expert_count = EXP_DEV * N_EP
    wide = tokens.astype(jnp.float32)
    ssq = lax.optimization_barrier(jnp.sum(wide * wide, axis=1, keepdims=True))
    normed = (wide * lax.rsqrt(ssq / D + norm_eps) * norm_gain[None, :]).astype(jnp.bfloat16)
    grouped = routing.reshape(N_EP, TOK_DEV * TOP)
    onehot = (grouped[:, :, None] == jnp.arange(expert_count, dtype=jnp.int32)[None, None, :]).astype(jnp.int32)
    slot_rank = lax.optimization_barrier(jnp.sum(jnp.cumsum(onehot, axis=1) * onehot, axis=2)) - 1
    groups = jnp.arange(N_EP, dtype=jnp.int32)[:, None]
    slot_index = (grouped * (N_EP * CAP) + groups * CAP + slot_rank).reshape(-1).astype(jnp.int32)
    repeated = jnp.repeat(normed, TOP, axis=0)
    buffer = jnp.zeros((expert_count * N_EP * CAP, D), jnp.bfloat16).at[slot_index].set(repeated)
    buffer = buffer.reshape(expert_count, N_EP * CAP, D)
    expert_out = lax.map(expert_apply, (buffer, w_gate, w_up, w_down))
    picked = expert_out.reshape(-1, D)[slot_index].astype(jnp.float32).reshape(TOKENS, TOP, D)
    mixed = lax.optimization_barrier(jnp.sum(gate_weights[:, :, None] * picked, axis=1))
    return mixed.astype(jnp.bfloat16)
```

```python
import functools

import jax
import jax.numpy as jnp
from jax import lax
from jax.experimental import pallas as pl
from jax.experimental.pallas import tpu as pltpu
from jax.sharding import PartitionSpec as P

CAP = 8
SIDE = 4
CORES = 2
PER = 4
FORWARD = False
DZS = (0, 1, -1, 2, 8, 7, -7, 6, -6, 5, -5, 4, -4, 3, -3, -2)
PLAN = ((7, 0), (7, 1), (0, 0), (7, 2), (0, 1), (1, 0), (7, 3), (0, 7), (0, 6), (1, 1), (1, 6), (3, 0), (1, 7), (0, 2), (0, 3), (0, 5), (0, 4), (3, 1), (3, 6), (3, 7), (1, 2), (1, 4), (5, 0), (1, 3), (1, 5), (5, 1), (5, 6), (5, 7), (6, 0), (3, 2), (3, 3), (3, 4), (6, 1), (6, 7), (3, 5), (6, 6), (5, 2), (5, 3), (5, 4), (5, 5), (6, 3), (6, 2), (6, 4), (6, 5))
COMBINE_AT = 6
MESH = pl.DeviceIdType.MESH

norm_eps = 1e-06
clamp_limit = 7.0
swish_alpha = 1.702


def arrangement(n_z):
    return [(dz % n_z, dc) for dz in DZS for dc in range(CORES)]


def kernel(
    n_ep,
    n_tp,
    tok_hbm,
    rout_hbm,
    gw_hbm,
    gain_hbm,
    wg_hbm,
    wu_hbm,
    wd_hbm,
    out_ref,
    tok_ref,
    rout_ref,
    gw_ref,
    gain_ref,
    wgu,
    wd,
    outgoing,
    rows,
    combine,
    part,
    far_in,
    near_in,
    light_in,
    ret_out,
    ret_in,
    in_sem,
    w_sem,
    disp_send,
    disp_recv,
    a_send,
    a_recv,
    b_send,
    b_recv,
    c_send,
    c_recv,
    far_send,
    far_recv,
    near_send,
    near_recv,
    light_send,
    light_recv,
    ret_send,
    ret_recv,
    open_sem,
):
    ep, tp = lax.axis_index("ep"), lax.axis_index("tp")
    n_exp, width, ff = wg_hbm.shape
    n_tok, cols = tok_ref.shape
    top = rout_ref.shape[0]
    chunk = n_exp * CAP
    slots = n_ep * chunk
    n_z = n_ep // CORES
    order = arrangement(n_z)
    groups = n_ep // PER
    block = PER * chunk
    z, core = ep // CORES, ep % CORES
    y, x = tp // SIDE, tp % SIDE

    def owner(p):
        dz, dc = order[p]
        return lax.rem(z + dz, n_z) * CORES + (1 - core if dc else core)

    def mirror(p):
        dz, dc = order[p]
        return order.index(((n_z - dz) % n_z, dc))

    def at(yy, xx):
        return lax.rem(yy, SIDE) * SIDE + lax.rem(xx, SIDE)

    small = [
        pltpu.make_async_copy(src, dst, in_sem.at[i])
        for i, (src, dst) in enumerate(
            ((rout_hbm, rout_ref), (gw_hbm, gw_ref), (tok_hbm, tok_ref), (gain_hbm, gain_ref))
        )
    ]
    for copy in small:
        copy.start()

    barrier = pltpu.get_barrier_semaphore()
    def reach(p):
        dz = order[p][0]
        return min(dz, n_z - dz)

    near = [p for p in range(1, n_ep) if reach(p) <= 1]
    for p in near:
        pl.semaphore_signal(barrier, inc=1, device_id=(owner(p), tp), device_id_type=MESH)
    for step in range(1, SIDE):
        pl.semaphore_signal(barrier, inc=1, device_id=(ep, at(y, x + step)), device_id_type=MESH)
        pl.semaphore_signal(barrier, inc=1, device_id=(ep, at(y + step, x)), device_id_type=MESH)

    loads = []
    for e in range(n_exp):
        for i, (src, dst) in enumerate(
            (
                (wg_hbm.at[e], wgu.at[e, :, pl.ds(0, ff)]),
                (wu_hbm.at[e], wgu.at[e, :, pl.ds(ff, ff)]),
                (wd_hbm.at[e], wd.at[e]),
            )
        ):
            loads.append(pltpu.make_async_copy(src, dst, w_sem.at[i, e]))
    for load in loads:
        load.start()

    slot_exp = jnp.concatenate(
        [
            owner(p) * n_exp + lax.broadcasted_iota(jnp.int32, (chunk, n_tok), 0) // CAP
            for p in range(n_ep)
        ],
        axis=0,
    )
    slot_rank = lax.broadcasted_iota(jnp.int32, (slots, n_tok), 0) % CAP
    named = jnp.zeros((slots, n_tok), jnp.float32)
    weight = jnp.zeros((slots, n_tok), jnp.float32)
    small[0].wait()
    small[1].wait()
    for k in range(top):
        hit = rout_ref[k : k + 1, :] == slot_exp
        named = named + jnp.where(hit, 1.0, 0.0)
        weight = weight + jnp.where(hit, gw_ref[k : k + 1, :], 0.0)
    earlier = jnp.where(
        lax.broadcasted_iota(jnp.int32, (n_tok, n_tok), 0)
        < lax.broadcasted_iota(jnp.int32, (n_tok, n_tok), 1),
        1.0,
        0.0,
    ).astype(jnp.bfloat16)
    rank = jnp.dot(named.astype(jnp.bfloat16), earlier, preferred_element_type=jnp.float32)
    placing = jnp.where(rank == slot_rank.astype(jnp.float32), named, 0.0)
    small[2].wait()
    sent = jnp.dot(
        placing.astype(jnp.bfloat16), tok_ref[...], preferred_element_type=jnp.float32
    ).astype(jnp.bfloat16)
    outgoing[...] = sent.reshape(n_ep, chunk, cols)
    rows[0, y, x, 0:chunk] = outgoing[0]


    def remote(src, dst, send, recv, peer):
        return pltpu.make_async_remote_copy(
            src_ref=src,
            dst_ref=dst,
            send_sem=send,
            recv_sem=recv,
            device_id=peer,
            device_id_type=MESH,
        )

    def dispatch(p, slot):
        g, s = divmod(slot, PER)
        return remote(
            outgoing.at[p],
            rows.at[g, y, x, pl.ds(s * chunk, chunk)],
            disp_send.at[p],
            disp_recv.at[slot],
            (owner(p), tp),
        )

    def heavy_y(g):
        return g % 2 == 0

    def place(g):
        return (y, x) if heavy_y(g) else (x, y)

    def peer(g, heavy, light):
        return (ep, at(heavy, light) if heavy_y(g) else at(light, heavy))

    def one(ref, g, heavy, light):
        heavy, light = lax.rem(heavy, SIDE), lax.rem(light, SIDE)
        return ref.at[g, heavy, light] if heavy_y(g) else ref.at[g, light, heavy]

    def line(ref, g, heavy, start=0, size=SIDE):
        heavy = lax.rem(heavy, SIDE)
        if heavy_y(g):
            return ref.at[g, heavy, pl.ds(start, size)]
        return ref.at[g, pl.ds(start, size), heavy]

    half = SIDE // 2
    steps = (1, SIDE - 1, 2)
    ways = (1, SIDE - 1) if FORWARD else steps
    n_ways = len(ways)

    def along_light(g, k):
        h, l = place(g)
        ref = one(rows, g, h, l)
        return remote(ref, ref, a_send.at[g, k], a_recv.at[g, k], peer(g, h, l + steps[k]))

    def along_heavy(g, k):
        h, l = place(g)
        ref = line(rows, g, h)
        return remote(ref, ref, b_send.at[g, k], b_recv.at[g, k], peer(g, h + ways[k], l))

    def pass_on(g, k):
        h, l = place(g)
        ref = line(rows, g, h + SIDE - ways[k], k * half, half)
        return remote(ref, ref, c_send.at[g, k], c_recv.at[g, k], peer(g, h + ways[k], l))

    def far_part(g, k):
        h, l = place(g)
        return remote(
            line(part, g, h + 2, k * half, half),
            far_in.at[g, k],
            far_send.at[g, k],
            far_recv.at[g, k],
            peer(g, h + ways[k], l),
        )

    def near_part(g, k, which):
        h, l = place(g)
        return remote(
            line(part, g, h + ways[k], which * half, half),
            near_in.at[g, k, pl.ds(which * half, half)],
            near_send.at[g, k, which],
            near_recv.at[g, k, which],
            peer(g, h + ways[k], l),
        )

    def whole_part(g, k):
        h, l = place(g)
        return remote(
            line(part, g, h + ways[k]),
            near_in.at[g, k],
            near_send.at[g, k, 0],
            near_recv.at[g, k, 0],
            peer(g, h + ways[k], l),
        )

    def light_part(g, k):
        h, l = place(g)
        return remote(
            one(part, g, h, l + steps[k]),
            light_in.at[g, k],
            light_send.at[g, k],
            light_recv.at[g, k],
            peer(g, h, l + steps[k]),
        )

    def give_back(p, slot):
        return remote(
            ret_out.at[p], ret_in.at[slot], ret_send.at[p], ret_recv.at[slot], (owner(p), tp)
        )

    hops = (1, 2, 4)

    def stage_open(k):
        if k == 0:
            pl.semaphore_wait(barrier, len(near) + 2 * (SIDE - 1))
        else:
            pl.semaphore_wait(open_sem.at[k - 1], 2)
        if k < len(hops):
            for d in (hops[k], n_z - hops[k]):
                pl.semaphore_signal(
                    open_sem.at[k],
                    inc=1,
                    device_id=(lax.rem(z + d, n_z) * CORES + core, tp),
                    device_id_type=MESH,
                )
        least = hops[k - 1] + 1 if k else 0
        most = 2 * least - 2 if k else 1
        for p in range(1, n_ep):
            if least <= reach(p) <= most:
                dispatch(p, mirror(p)).start()

    def stage_take(g):
        for p in range(g * PER, (g + 1) * PER):
            if p:
                dispatch(p, p).wait_recv()
        for k in range(3):
            along_light(g, k).start()

    def stage_spread(g):
        for k in range(3):
            along_light(g, k).wait_recv()
        for k in range(n_ways):
            along_heavy(g, k).start()

    def stage_pass(g):
        for k in range(2):
            along_heavy(g, k).wait_recv()
            pass_on(g, k).start()

    def stage_compute(g):
        if FORWARD:
            for k in range(2):
                pass_on(g, k).wait_recv()
        else:
            for k in range(n_ways):
                along_heavy(g, k).wait_recv()
        if g == 0:
            small[3].wait()
        ssq = jnp.zeros((block, cols), jnp.float32)
        xs = [[] for _ in range(n_exp)]
        for j in range(n_tp):
            wide = rows[g, j // SIDE, j % SIDE].astype(jnp.float32)
            ssq = ssq + wide * wide
            scaled = (wide * gain_ref[:, j * cols : (j + 1) * cols]).reshape(
                PER, n_exp, CAP, cols
            )
            for e in range(n_exp):
                xs[e].append(scaled[:, e].reshape(PER * CAP, cols).astype(jnp.bfloat16))
        total = jnp.sum(ssq, axis=1, keepdims=True)
        scale = lax.rsqrt(total / width + norm_eps).reshape(PER, n_exp, CAP, 1)
        for e in range(n_exp):
            if g == 0:
                for i in range(3):
                    loads[3 * e + i].wait()
            pre = jnp.dot(
                jnp.concatenate(xs[e], axis=1), wgu[e], preferred_element_type=jnp.float32
            )
            pre = pre * scale[:, e].reshape(PER * CAP, 1)
            clamped = jnp.minimum(pre[:, :ff], clamp_limit)
            upper = jnp.clip(pre[:, ff:], -clamp_limit, clamp_limit)
            hidden = (clamped * jax.nn.sigmoid(swish_alpha * clamped) * (upper + 1.0)).astype(
                jnp.bfloat16
            )
            down = jnp.dot(hidden, wd[e], preferred_element_type=jnp.float32).astype(
                jnp.bfloat16
            )
            for q in range(n_tp):
                part[g, q // SIDE, q % SIDE, e * PER * CAP : (e + 1) * PER * CAP] = down[
                    :, q * cols : (q + 1) * cols
                ]
        if FORWARD:
            for k in range(2):
                far_part(g, k).start()
                near_part(g, k, 1 - k).start()
        else:
            for k in range(n_ways):
                whole_part(g, k).start()

    def stage_join(g):
        h, l = place(g)
        for k in range(2):
            far_part(g, k).wait_recv()
            mine = line(part, g, h + ways[k], k * half, half)
            mine[...] = (
                mine[...].astype(jnp.float32) + far_in[g, k].astype(jnp.float32)
            ).astype(jnp.bfloat16)
            near_part(g, k, k).start()

    def stage_sum(g):
        h, l = place(g)
        mine = line(part, g, h)
        total = mine[...].astype(jnp.float32)
        for k in range(n_ways):
            if FORWARD:
                for which in range(2):
                    near_part(g, k, which).wait_recv()
            else:
                whole_part(g, k).wait_recv()
            total = total + near_in[g, k].astype(jnp.float32)
        mine[...] = total.astype(jnp.bfloat16)
        for k in range(3):
            light_part(g, k).start()

    def stage_return(g):
        h, l = place(g)
        total = one(part, g, h, l)[...].astype(jnp.float32)
        for k in range(3):
            light_part(g, k).wait_recv()
            total = total + light_in[g, k].astype(jnp.float32)
        total = total.reshape(n_exp, PER, CAP, cols)
        back = jnp.stack([total[e] for e in range(n_exp)], axis=1).reshape(PER, chunk, cols)
        ret_out[g * PER : (g + 1) * PER] = back.astype(jnp.bfloat16)
        for p in range(g * PER, (g + 1) * PER):
            if p:
                give_back(p, mirror(p)).start()
            else:
                ret_in[0] = ret_out[0]


    stages = (
        stage_take,
        stage_spread,
        stage_pass,
        stage_compute,
        stage_join,
        stage_sum,
        stage_return,
        stage_open,
    )
    for step, (stage, g) in enumerate(PLAN):
        stages[stage](g)
        if step == COMBINE_AT:
            combine[...] = (placing * weight).T

    both = combine[...]
    high = both.astype(jnp.bfloat16)
    low = (both - high.astype(jnp.float32)).astype(jnp.bfloat16)

    for p in range(1, n_ep):
        dispatch(p, mirror(p)).wait_send()
    for g in range(groups):
        for k in range(3):
            along_light(g, k).wait_send()
            light_part(g, k).wait_send()
        for k in range(n_ways):
            along_heavy(g, k).wait_send()
            if FORWARD:
                pass_on(g, k).wait_send()
                far_part(g, k).wait_send()
                for which in range(2):
                    near_part(g, k, which).wait_send()
            else:
                whole_part(g, k).wait_send()
    for p in range(1, n_ep):
        give_back(p, p).wait_recv()
    back = ret_in[...].reshape(slots, cols)
    out_ref[...] = (
        jnp.dot(high, back, preferred_element_type=jnp.float32)
        + jnp.dot(low, back, preferred_element_type=jnp.float32)
    ).astype(jnp.bfloat16)
    for p in range(1, n_ep):
        give_back(p, mirror(p)).wait_send()


def per_device(tokens, routing, gate_weights, norm_gain, w_gate, w_up, w_down):
    n_ep, n_tp = lax.axis_size("ep"), lax.axis_size("tp")
    n_exp, width, ff = w_gate.shape
    n_tok, cols = tokens.shape
    chunk = n_exp * CAP
    slots = n_ep * chunk
    groups, block = n_ep // PER, PER * chunk
    vmem = pl.BlockSpec(memory_space=pltpu.VMEM)
    hbm = pl.BlockSpec(memory_space=pltpu.HBM)
    bf16, f32 = jnp.bfloat16, jnp.float32
    dma = pltpu.SemaphoreType.DMA
    return pl.pallas_call(
        functools.partial(kernel, n_ep, n_tp),
        out_shape=jax.ShapeDtypeStruct((n_tok, cols), bf16),
        in_specs=[hbm] * 7,
        out_specs=vmem,
        scratch_shapes=[
            pltpu.VMEM(tokens.shape, bf16),
            pltpu.VMEM(routing.shape[::-1], jnp.int32),
            pltpu.VMEM(gate_weights.shape[::-1], f32),
            pltpu.VMEM((1, width), f32),
            pltpu.VMEM((n_exp, width, 2 * ff), bf16),
            pltpu.VMEM(w_down.shape, bf16),
            pltpu.VMEM((n_ep, chunk, cols), bf16),
            pltpu.VMEM((groups, SIDE, SIDE, block, cols), bf16),
            pltpu.VMEM((n_tok, slots), f32),
            pltpu.VMEM((groups, SIDE, SIDE, block, cols), bf16),
            pltpu.VMEM((groups, 2, SIDE // 2, block, cols), bf16),
            pltpu.VMEM((groups, 3, SIDE, block, cols), bf16),
            pltpu.VMEM((groups, 3, block, cols), bf16),
            pltpu.VMEM((n_ep, chunk, cols), bf16),
            pltpu.VMEM((n_ep, chunk, cols), bf16),
            dma((4,)),
            dma((3, n_exp)),
            dma((n_ep,)),
            dma((n_ep,)),
            dma((groups, 3)),
            dma((groups, 3)),
            dma((groups, 3)),
            dma((groups, 3)),
            dma((groups, 2)),
            dma((groups, 2)),
            dma((groups, 2)),
            dma((groups, 2)),
            dma((groups, 3, 2)),
            dma((groups, 3, 2)),
            dma((groups, 3)),
            dma((groups, 3)),
            dma((n_ep,)),
            dma((n_ep,)),
            pltpu.SemaphoreType.REGULAR((3,)),
        ],
        compiler_params=pltpu.CompilerParams(collective_id=0, has_side_effects=True),
    )(tokens, routing.T, gate_weights.T, norm_gain.reshape(1, width), w_gate, w_up, w_down)


def solution(mesh):
    in_specs = (
        P("ep", "tp"),
        P("ep", None),
        P("ep", None),
        P(),
        P("ep", None, "tp"),
        P("ep", None, "tp"),
        P("ep", "tp", None),
    )
    return jax.shard_map(
        per_device, mesh=mesh, in_specs=in_specs, out_specs=P("ep", "tp"), check_vma=False
    )
```

```python
import functools

import jax
import jax.numpy as jnp
from jax import lax
from jax.experimental import pallas as pl
from jax.experimental.pallas import tpu as pltpu
from jax.sharding import PartitionSpec as P

CAP = 8
SIDE = 4
CORES = 2
PER = 4
DZS = (0, 1, -1, 2, -2, 3, -3, 4, 8, 7, -7, 6, -6, 5, -5, -4)
PLAN = ((0, 0), (0, 1), (0, 2), (0, 3), (1, 0), (0, 7), (0, 6), (0, 5), (1, 1), (0, 4), (1, 2), (1, 3), (2, 0), (1, 6), (2, 1), (1, 7), (1, 5), (1, 4), (2, 2), (2, 3), (3, 0), (3, 1), (2, 6), (2, 7), (2, 4), (2, 5), (3, 2), (3, 3), (4, 0), (4, 1), (3, 6), (3, 7), (3, 4), (3, 5), (4, 2), (4, 3), (5, 0), (5, 1), (4, 6), (4, 7), (4, 4), (4, 5), (5, 2), (5, 3), (6, 1), (5, 6), (6, 0), (5, 7), (5, 4), (5, 5), (6, 2), (6, 3), (6, 6), (6, 7), (6, 4), (6, 5))
COMBINE_AT = 6
MESH = pl.DeviceIdType.MESH

norm_eps = 1e-06
clamp_limit = 7.0
swish_alpha = 1.702


def arrangement(n_z):
    return [(dz % n_z, dc) for dz in DZS for dc in range(CORES)]


def kernel(
    n_ep,
    n_tp,
    tok_hbm,
    rout_hbm,
    gw_hbm,
    gain_hbm,
    wg_hbm,
    wu_hbm,
    wd_hbm,
    out_ref,
    tok_ref,
    rout_ref,
    gw_ref,
    gain_ref,
    wgu,
    wd,
    outgoing,
    rows,
    combine,
    part,
    far_in,
    near_in,
    light_in,
    ret_out,
    ret_in,
    in_sem,
    w_sem,
    disp_send,
    disp_recv,
    a_send,
    a_recv,
    b_send,
    b_recv,
    c_send,
    c_recv,
    far_send,
    far_recv,
    near_send,
    near_recv,
    light_send,
    light_recv,
    ret_send,
    ret_recv,
):
    ep, tp = lax.axis_index("ep"), lax.axis_index("tp")
    n_exp, width, ff = wg_hbm.shape
    n_tok, cols = tok_ref.shape
    top = rout_ref.shape[0]
    chunk = n_exp * CAP
    slots = n_ep * chunk
    n_z = n_ep // CORES
    order = arrangement(n_z)
    groups = n_ep // PER
    block = PER * chunk
    z, core = ep // CORES, ep % CORES
    y, x = tp // SIDE, tp % SIDE

    def owner(p):
        dz, dc = order[p]
        return lax.rem(z + dz, n_z) * CORES + (1 - core if dc else core)

    def mirror(p):
        dz, dc = order[p]
        return order.index(((n_z - dz) % n_z, dc))

    def at(yy, xx):
        return lax.rem(yy, SIDE) * SIDE + lax.rem(xx, SIDE)

    small = [
        pltpu.make_async_copy(src, dst, in_sem.at[i])
        for i, (src, dst) in enumerate(
            ((rout_hbm, rout_ref), (gw_hbm, gw_ref), (tok_hbm, tok_ref), (gain_hbm, gain_ref))
        )
    ]
    for copy in small:
        copy.start()

    barrier = pltpu.get_barrier_semaphore()
    for p in reversed(range(1, n_ep)):
        pl.semaphore_signal(barrier, inc=1, device_id=(owner(p), tp), device_id_type=MESH)
    for step in range(1, SIDE):
        pl.semaphore_signal(barrier, inc=1, device_id=(ep, at(y, x + step)), device_id_type=MESH)
        pl.semaphore_signal(barrier, inc=1, device_id=(ep, at(y + step, x)), device_id_type=MESH)

    loads = []
    for e in range(n_exp):
        for i, (src, dst) in enumerate(
            (
                (wg_hbm.at[e], wgu.at[e, :, pl.ds(0, ff)]),
                (wu_hbm.at[e], wgu.at[e, :, pl.ds(ff, ff)]),
                (wd_hbm.at[e], wd.at[e]),
            )
        ):
            loads.append(pltpu.make_async_copy(src, dst, w_sem.at[i, e]))
    for load in loads:
        load.start()

    which = jnp.concatenate([jnp.full((CAP, n_tok), e, jnp.int32) for e in range(n_exp)], axis=0)
    slot_exp = jnp.concatenate(
        [
            owner(p) * n_exp + which
            for p in range(n_ep)
        ],
        axis=0,
    )
    slot_rank = lax.broadcasted_iota(jnp.int32, (slots, n_tok), 0) & (CAP - 1)
    named = jnp.zeros((slots, n_tok), jnp.float32)
    small[0].wait()
    for k in range(top):
        hit = rout_ref[k : k + 1, :] == slot_exp
        named = named + jnp.where(hit, 1.0, 0.0)
    earlier = jnp.where(
        lax.broadcasted_iota(jnp.int32, (n_tok, n_tok), 0)
        < lax.broadcasted_iota(jnp.int32, (n_tok, n_tok), 1),
        1.0,
        0.0,
    ).astype(jnp.bfloat16)
    rank = jnp.dot(named.astype(jnp.bfloat16), earlier, preferred_element_type=jnp.float32)
    placing = jnp.where(rank == slot_rank.astype(jnp.float32), named, 0.0)
    small[2].wait()
    sent = jnp.dot(
        placing.astype(jnp.bfloat16), tok_ref[...], preferred_element_type=jnp.float32
    ).astype(jnp.bfloat16)
    outgoing[...] = sent.reshape(n_ep, chunk, cols)
    rows[0, y, x, 0:chunk] = outgoing[0]


    def remote(src, dst, send, recv, peer):
        return pltpu.make_async_remote_copy(
            src_ref=src,
            dst_ref=dst,
            send_sem=send,
            recv_sem=recv,
            device_id=peer,
            device_id_type=MESH,
        )

    def dispatch(p, slot):
        g, s = divmod(slot, PER)
        return remote(
            outgoing.at[p],
            rows.at[g, y, x, pl.ds(s * chunk, chunk)],
            disp_send,
            disp_recv.at[g],
            (owner(p), tp),
        )

    def heavy_y(g):
        return g % 2 == 0

    def place(g):
        return (y, x) if heavy_y(g) else (x, y)

    def peer(g, heavy, light):
        return (ep, at(heavy, light) if heavy_y(g) else at(light, heavy))

    def one(ref, g, heavy, light):
        heavy, light = lax.rem(heavy, SIDE), lax.rem(light, SIDE)
        return ref.at[g, heavy, light] if heavy_y(g) else ref.at[g, light, heavy]

    def line(ref, g, heavy, start=0, size=SIDE):
        heavy = lax.rem(heavy, SIDE)
        if heavy_y(g):
            return ref.at[g, heavy, pl.ds(start, size)]
        return ref.at[g, pl.ds(start, size), heavy]

    half = SIDE // 2
    steps = (1, SIDE - 1, 2)
    ways = (1, SIDE - 1)

    def along_light(g, k):
        h, l = place(g)
        ref = one(rows, g, h, l)
        return remote(ref, ref, a_send, a_recv.at[g], peer(g, h, l + steps[k]))

    def along_heavy(g, k):
        h, l = place(g)
        ref = line(rows, g, h)
        return remote(ref, ref, b_send, b_recv.at[g, k], peer(g, h + ways[k], l))

    def pass_on(g, k):
        h, l = place(g)
        ref = line(rows, g, h + SIDE - ways[k], k * half, half)
        return remote(ref, ref, c_send, c_recv.at[g], peer(g, h + ways[k], l))

    def far_part(g, k):
        h, l = place(g)
        return remote(
            line(part, g, h + 2, k * half, half),
            far_in.at[g, k],
            far_send,
            far_recv.at[g],
            peer(g, h + ways[k], l),
        )

    def near_part(g, k, which):
        h, l = place(g)
        return remote(
            line(part, g, h + ways[k], which * half, half),
            near_in.at[g, k, pl.ds(which * half, half)],
            near_send,
            near_recv.at[g],
            peer(g, h + ways[k], l),
        )

    def light_part(g, k):
        h, l = place(g)
        return remote(
            one(part, g, h, l + steps[k]),
            light_in.at[g, k],
            light_send,
            light_recv.at[g],
            peer(g, h, l + steps[k]),
        )

    def give_back(p, slot):
        return remote(
            ret_out.at[p], ret_in.at[slot], ret_send, ret_recv, (owner(p), tp)
        )

    def arrived(ref, recv):
        remote(ref, ref, disp_send, recv, (ep, tp)).wait_recv()

    def left(ref, send):
        remote(ref, ref, send, ret_recv, (ep, tp)).wait_send()

    def stage_take(g):
        own = 0 if g else chunk
        arrived(rows.at[g, y, x, pl.ds(own, block - own)], disp_recv.at[g])
        for k in range(3):
            along_light(g, k).start()

    def stage_spread(g):
        arrived(rows.at[g, 0, pl.ds(0, len(steps))], a_recv.at[g])
        for k in range(2):
            along_heavy(g, k).start()

    def stage_pass(g):
        for k in range(2):
            along_heavy(g, k).wait_recv()
            pass_on(g, k).start()

    def stage_compute(g):
        arrived(rows.at[g, 0], c_recv.at[g])
        if g == 0:
            small[3].wait()
        ssq = jnp.zeros((block, cols), jnp.float32)
        xs = [[] for _ in range(n_exp)]
        for j in range(n_tp):
            wide = rows[g, j // SIDE, j % SIDE].astype(jnp.float32)
            ssq = ssq + wide * wide
            scaled = (wide * gain_ref[:, j * cols : (j + 1) * cols]).reshape(
                PER, n_exp, CAP, cols
            )
            for e in range(n_exp):
                xs[e].append(scaled[:, e].reshape(PER * CAP, cols).astype(jnp.bfloat16))
        total = jnp.sum(ssq, axis=1, keepdims=True)
        scale = lax.rsqrt(total / width + norm_eps).reshape(PER, n_exp, CAP, 1)
        for e in range(n_exp):
            if g == 0:
                for i in range(3):
                    loads[3 * e + i].wait()
            pre = jnp.dot(
                jnp.concatenate(xs[e], axis=1), wgu[e], preferred_element_type=jnp.float32
            )
            pre = pre * scale[:, e].reshape(PER * CAP, 1)
            clamped = jnp.minimum(pre[:, :ff], clamp_limit)
            upper = jnp.clip(pre[:, ff:], -clamp_limit, clamp_limit)
            hidden = (clamped * jax.nn.sigmoid(swish_alpha * clamped) * (upper + 1.0)).astype(
                jnp.bfloat16
            )
            down = jnp.dot(hidden, wd[e], preferred_element_type=jnp.float32).astype(
                jnp.bfloat16
            )
            for q in range(n_tp):
                part[g, q // SIDE, q % SIDE, e * PER * CAP : (e + 1) * PER * CAP] = down[
                    :, q * cols : (q + 1) * cols
                ]
        for k in range(2):
            far_part(g, k).start()
            near_part(g, k, 1 - k).start()

    def stage_join(g):
        h, l = place(g)
        arrived(far_in.at[g], far_recv.at[g])
        for k in range(2):
            mine = line(part, g, h + ways[k], k * half, half)
            mine[...] = (
                mine[...].astype(jnp.float32) + far_in[g, k].astype(jnp.float32)
            ).astype(jnp.bfloat16)
            near_part(g, k, k).start()

    def stage_sum(g):
        h, l = place(g)
        mine = line(part, g, h)
        total = mine[...].astype(jnp.float32)
        arrived(near_in.at[g], near_recv.at[g])
        for k in range(2):
            total = total + near_in[g, k].astype(jnp.float32)
        mine[...] = total.astype(jnp.bfloat16)
        for k in range(3):
            light_part(g, k).start()

    def stage_return(g):
        h, l = place(g)
        total = one(part, g, h, l)[...].astype(jnp.float32)
        arrived(light_in.at[g], light_recv.at[g])
        for k in range(3):
            total = total + light_in[g, k].astype(jnp.float32)
        total = total.reshape(n_exp, PER, CAP, cols)
        back = jnp.stack([total[e] for e in range(n_exp)], axis=1).reshape(PER, chunk, cols)
        ret_out[g * PER : (g + 1) * PER] = back.astype(jnp.bfloat16)
        for p in range(g * PER, (g + 1) * PER):
            if p:
                give_back(p, mirror(p)).start()
            else:
                ret_in[0] = ret_out[0]


    stages = (
        stage_take,
        stage_spread,
        stage_pass,
        stage_compute,
        stage_join,
        stage_sum,
        stage_return,
    )
    pl.semaphore_wait(barrier, n_ep - 1 + 2 * (SIDE - 1))
    for p in range(1, n_ep):
        dispatch(p, mirror(p)).start()
    for step, (stage, g) in enumerate(PLAN):
        stages[stage](g)
        if step == COMBINE_AT:
            small[1].wait()
            weight = jnp.zeros((slots, n_tok), jnp.float32)
            for k in range(top):
                hit = rout_ref[k : k + 1, :] == slot_exp
                weight = weight + jnp.where(hit, gw_ref[k : k + 1, :], 0.0)
            combine[...] = (placing * weight).T

    both = combine[...]
    high = both.astype(jnp.bfloat16)
    low = (both - high.astype(jnp.float32)).astype(jnp.bfloat16)

    others = pl.ds(1, n_ep - 1)
    left(outgoing.at[others], disp_send)
    most = groups * len(steps) // SIDE
    left(rows.at[pl.ds(0, most), 0], a_send)
    left(rows.at[:, pl.ds(0, 2)], b_send)
    left(rows.at[:, 0], c_send)
    left(far_in, far_send)
    left(near_in, near_send)
    left(light_in, light_send)
    arrived(ret_in.at[others], ret_recv)
    back = ret_in[...].reshape(slots, cols)
    out_ref[...] = (
        jnp.dot(high, back, preferred_element_type=jnp.float32)
        + jnp.dot(low, back, preferred_element_type=jnp.float32)
    ).astype(jnp.bfloat16)
    left(ret_out.at[others], ret_send)


def per_device(tokens, routing, gate_weights, norm_gain, w_gate, w_up, w_down):
    n_ep, n_tp = lax.axis_size("ep"), lax.axis_size("tp")
    n_exp, width, ff = w_gate.shape
    n_tok, cols = tokens.shape
    chunk = n_exp * CAP
    slots = n_ep * chunk
    groups, block = n_ep // PER, PER * chunk
    vmem = pl.BlockSpec(memory_space=pltpu.VMEM)
    hbm = pl.BlockSpec(memory_space=pltpu.HBM)
    bf16, f32 = jnp.bfloat16, jnp.float32
    dma = pltpu.SemaphoreType.DMA
    return pl.pallas_call(
        functools.partial(kernel, n_ep, n_tp),
        out_shape=jax.ShapeDtypeStruct((n_tok, cols), bf16),
        in_specs=[hbm] * 7,
        out_specs=vmem,
        scratch_shapes=[
            pltpu.VMEM(tokens.shape, bf16),
            pltpu.VMEM(routing.shape[::-1], jnp.int32),
            pltpu.VMEM(gate_weights.shape[::-1], f32),
            pltpu.VMEM((1, width), f32),
            pltpu.VMEM((n_exp, width, 2 * ff), bf16),
            pltpu.VMEM(w_down.shape, bf16),
            pltpu.VMEM((n_ep, chunk, cols), bf16),
            pltpu.VMEM((groups, SIDE, SIDE, block, cols), bf16),
            pltpu.VMEM((n_tok, slots), f32),
            pltpu.VMEM((groups, SIDE, SIDE, block, cols), bf16),
            pltpu.VMEM((groups, 2, SIDE // 2, block, cols), bf16),
            pltpu.VMEM((groups, 2, SIDE, block, cols), bf16),
            pltpu.VMEM((groups, 3, block, cols), bf16),
            pltpu.VMEM((n_ep, chunk, cols), bf16),
            pltpu.VMEM((n_ep, chunk, cols), bf16),
            dma((4,)),
            dma((3, n_exp)),
            dma,
            dma((groups,)),
            dma,
            dma((groups,)),
            dma,
            dma((groups, 2)),
            dma,
            dma((groups,)),
            dma,
            dma((groups,)),
            dma,
            dma((groups,)),
            dma,
            dma((groups,)),
            dma,
            dma,
        ],
        compiler_params=pltpu.CompilerParams(collective_id=0, has_side_effects=True),
    )(tokens, routing.T, gate_weights.T, norm_gain.reshape(1, width), w_gate, w_up, w_down)


def solution(mesh):
    in_specs = (
        P("ep", "tp"),
        P("ep", None),
        P("ep", None),
        P(),
        P("ep", None, "tp"),
        P("ep", None, "tp"),
        P("ep", "tp", None),
    )
    return jax.shard_map(
        per_device, mesh=mesh, in_specs=in_specs, out_specs=P("ep", "tp"), check_vma=False
    )
```

```python
import functools

import jax
import jax.numpy as jnp
from jax import lax
from jax.experimental import pallas as pl
from jax.experimental.pallas import tpu as pltpu
from jax.sharding import PartitionSpec as P

CAP = 8
SIDE = 4
CORES = 2
PER = 4
DZS = (0, 1, -1, 2, -2, 3, -3, 4, 8, 7, -7, 6, -6, 5, -5, -4)
PLAN = ((0, 0), (0, 1), (0, 2), (0, 3), (1, 0), (1, 1), (0, 4), (0, 5), (0, 6), (0, 7), (1, 2), (1, 3), (2, 0), (2, 1), (1, 4), (1, 5), (2, 2), (1, 6), (1, 7), (3, 0), (2, 3), (3, 1), (2, 4), (2, 5), (3, 2), (2, 6), (2, 7), (3, 3), (4, 0), (4, 1), (3, 4), (3, 5), (4, 2), (4, 3), (3, 6), (3, 7), (5, 0), (5, 1), (4, 4), (4, 5), (5, 2), (5, 3), (4, 6), (4, 7), (5, 4), (6, 0), (6, 1), (5, 5), (5, 6), (6, 2), (6, 3), (5, 7), (6, 4), (6, 5), (6, 6), (6, 7))
COMBINE_AT = 6
MESH = pl.DeviceIdType.MESH

norm_eps = 1e-06
clamp_limit = 7.0
swish_alpha = 1.702


def arrangement(n_z):
    return [(dz % n_z, dc) for dz in DZS for dc in range(CORES)]


def kernel(
    n_ep,
    n_tp,
    tok_hbm,
    rout_hbm,
    gw_hbm,
    gain_hbm,
    wg_hbm,
    wu_hbm,
    wd_hbm,
    out_ref,
    tok_ref,
    rout_ref,
    gw_ref,
    gain_ref,
    wgu,
    wd,
    outgoing,
    rows,
    combine,
    part,
    far_in,
    near_in,
    light_in,
    ret_out,
    ret_in,
    in_sem,
    w_sem,
    disp_send,
    disp_recv,
    a_send,
    a_recv,
    b_send,
    b_recv,
    c_send,
    c_recv,
    far_send,
    far_recv,
    near_send,
    near_recv,
    light_send,
    light_recv,
    ret_send,
    ret_recv,
):
    ep, tp = lax.axis_index("ep"), lax.axis_index("tp")
    n_exp, width, ff = wg_hbm.shape
    n_tok, cols = tok_ref.shape
    top = rout_ref.shape[0]
    chunk = n_exp * CAP
    slots = n_ep * chunk
    n_z = n_ep // CORES
    order = arrangement(n_z)
    groups = n_ep // PER
    block = PER * chunk
    z, core = ep // CORES, ep % CORES
    y, x = tp // SIDE, tp % SIDE

    def owner(p):
        dz, dc = order[p]
        return lax.rem(z + dz, n_z) * CORES + (1 - core if dc else core)

    def mirror(p):
        dz, dc = order[p]
        return order.index(((n_z - dz) % n_z, dc))

    def at(yy, xx):
        return lax.rem(yy, SIDE) * SIDE + lax.rem(xx, SIDE)

    small = [
        pltpu.make_async_copy(src, dst, in_sem.at[i])
        for i, (src, dst) in enumerate(
            ((rout_hbm, rout_ref), (gw_hbm, gw_ref), (tok_hbm, tok_ref), (gain_hbm, gain_ref))
        )
    ]
    for copy in small:
        copy.start()

    barrier = pltpu.get_barrier_semaphore()
    for p in reversed(range(1, n_ep)):
        pl.semaphore_signal(barrier, inc=1, device_id=(owner(p), tp), device_id_type=MESH)
    for step in range(1, SIDE):
        pl.semaphore_signal(barrier, inc=1, device_id=(ep, at(y, x + step)), device_id_type=MESH)
        pl.semaphore_signal(barrier, inc=1, device_id=(ep, at(y + step, x)), device_id_type=MESH)

    loads = []
    for e in range(n_exp):
        for i, (src, dst) in enumerate(
            (
                (wg_hbm.at[e], wgu.at[e, :, pl.ds(0, ff)]),
                (wu_hbm.at[e], wgu.at[e, :, pl.ds(ff, ff)]),
                (wd_hbm.at[e], wd.at[e]),
            )
        ):
            loads.append(pltpu.make_async_copy(src, dst, w_sem.at[i, e]))
    for load in loads:
        load.start()

    which = jnp.concatenate([jnp.full((CAP, n_tok), e, jnp.int32) for e in range(n_exp)], axis=0)
    slot_exp = jnp.concatenate(
        [
            owner(p) * n_exp + which
            for p in range(n_ep)
        ],
        axis=0,
    )
    slot_rank = lax.broadcasted_iota(jnp.int32, (slots, n_tok), 0) & (CAP - 1)
    named = jnp.zeros((slots, n_tok), jnp.float32)
    small[0].wait()
    for k in range(top):
        hit = rout_ref[k : k + 1, :] == slot_exp
        named = named + jnp.where(hit, 1.0, 0.0)
    earlier = jnp.where(
        lax.broadcasted_iota(jnp.int32, (n_tok, n_tok), 0)
        < lax.broadcasted_iota(jnp.int32, (n_tok, n_tok), 1),
        1.0,
        0.0,
    ).astype(jnp.bfloat16)
    rank = jnp.dot(named.astype(jnp.bfloat16), earlier, preferred_element_type=jnp.float32)
    placing = jnp.where(rank == slot_rank.astype(jnp.float32), named, 0.0)
    small[2].wait()
    sent = jnp.dot(
        placing.astype(jnp.bfloat16), tok_ref[...], preferred_element_type=jnp.float32
    ).astype(jnp.bfloat16)
    outgoing[...] = sent.reshape(n_ep, chunk, cols)
    rows[0, y, x, 0:chunk] = outgoing[0]


    def remote(src, dst, send, recv, peer):
        return pltpu.make_async_remote_copy(
            src_ref=src,
            dst_ref=dst,
            send_sem=send,
            recv_sem=recv,
            device_id=peer,
            device_id_type=MESH,
        )

    def dispatch(p, slot):
        g, s = divmod(slot, PER)
        return remote(
            outgoing.at[p],
            rows.at[g, y, x, pl.ds(s * chunk, chunk)],
            disp_send,
            disp_recv.at[g],
            (owner(p), tp),
        )

    def heavy_y(g):
        return g % 2 == 0

    def place(g):
        return (y, x) if heavy_y(g) else (x, y)

    def peer(g, heavy, light):
        return (ep, at(heavy, light) if heavy_y(g) else at(light, heavy))

    def one(ref, g, heavy, light):
        heavy, light = lax.rem(heavy, SIDE), lax.rem(light, SIDE)
        return ref.at[g, heavy, light] if heavy_y(g) else ref.at[g, light, heavy]

    def line(ref, g, heavy, start=0, size=SIDE):
        heavy = lax.rem(heavy, SIDE)
        if heavy_y(g):
            return ref.at[g, heavy, pl.ds(start, size)]
        return ref.at[g, pl.ds(start, size), heavy]

    half = SIDE // 2
    steps = (1, SIDE - 1, 2)
    ways = (1, SIDE - 1)

    def along_light(g, k):
        h, l = place(g)
        ref = one(rows, g, h, l)
        return remote(ref, ref, a_send, a_recv.at[g], peer(g, h, l + steps[k]))

    def along_heavy(g, k):
        h, l = place(g)
        ref = line(rows, g, h)
        return remote(ref, ref, b_send, b_recv.at[g, k], peer(g, h + ways[k], l))

    def pass_on(g, k):
        h, l = place(g)
        ref = line(rows, g, h + SIDE - ways[k], k * half, half)
        return remote(ref, ref, c_send, c_recv.at[g], peer(g, h + ways[k], l))

    def far_part(g, k):
        h, l = place(g)
        return remote(
            line(part, g, h + 2, k * half, half),
            far_in.at[g, k],
            far_send,
            far_recv.at[g],
            peer(g, h + ways[k], l),
        )

    def near_part(g, k, which):
        h, l = place(g)
        return remote(
            line(part, g, h + ways[k], which * half, half),
            near_in.at[g, k, pl.ds(which * half, half)],
            near_send,
            near_recv.at[g],
            peer(g, h + ways[k], l),
        )

    def light_part(g, k):
        h, l = place(g)
        return remote(
            one(part, g, h, l + steps[k]),
            light_in.at[g, k],
            light_send,
            light_recv.at[g],
            peer(g, h, l + steps[k]),
        )

    def give_back(p, slot):
        return remote(
            ret_out.at[p], ret_in.at[slot], ret_send, ret_recv, (owner(p), tp)
        )

    def arrived(ref, recv):
        remote(ref, ref, disp_send, recv, (ep, tp)).wait_recv()

    def left(ref, send):
        remote(ref, ref, send, ret_recv, (ep, tp)).wait_send()

    def stage_take(g):
        own = 0 if g else chunk
        arrived(rows.at[g, y, x, pl.ds(own, block - own)], disp_recv.at[g])
        for k in range(3):
            along_light(g, k).start()

    def stage_spread(g):
        arrived(rows.at[g, 0, pl.ds(0, len(steps))], a_recv.at[g])
        for k in range(2):
            along_heavy(g, k).start()

    def stage_pass(g):
        for k in range(2):
            along_heavy(g, k).wait_recv()
            pass_on(g, k).start()

    def stage_compute(g):
        arrived(rows.at[g, 0], c_recv.at[g])
        if g == 0:
            small[3].wait()
        ssq = jnp.zeros((block, cols), jnp.float32)
        xs = [[] for _ in range(n_exp)]
        for j in range(n_tp):
            wide = rows[g, j // SIDE, j % SIDE].astype(jnp.float32)
            ssq = ssq + wide * wide
            scaled = (wide * gain_ref[:, j * cols : (j + 1) * cols]).reshape(
                PER, n_exp, CAP, cols
            )
            for e in range(n_exp):
                xs[e].append(scaled[:, e].reshape(PER * CAP, cols).astype(jnp.bfloat16))
        total = jnp.sum(ssq, axis=1, keepdims=True)
        scale = lax.rsqrt(total / width + norm_eps).reshape(PER, n_exp, CAP, 1)
        for e in range(n_exp):
            if g == 0:
                for i in range(3):
                    loads[3 * e + i].wait()
            pre = jnp.dot(
                jnp.concatenate(xs[e], axis=1), wgu[e], preferred_element_type=jnp.float32
            )
            pre = pre * scale[:, e].reshape(PER * CAP, 1)
            clamped = jnp.minimum(pre[:, :ff], clamp_limit)
            upper = jnp.clip(pre[:, ff:], -clamp_limit, clamp_limit)
            hidden = (clamped * jax.nn.sigmoid(swish_alpha * clamped) * (upper + 1.0)).astype(
                jnp.bfloat16
            )
            down = jnp.dot(hidden, wd[e], preferred_element_type=jnp.float32).astype(
                jnp.bfloat16
            )
            for q in range(n_tp):
                part[g, q // SIDE, q % SIDE, e * PER * CAP : (e + 1) * PER * CAP] = down[
                    :, q * cols : (q + 1) * cols
                ]
        for k in range(2):
            far_part(g, k).start()
            near_part(g, k, 1 - k).start()

    def stage_join(g):
        h, l = place(g)
        arrived(far_in.at[g], far_recv.at[g])
        for k in range(2):
            mine = line(part, g, h + ways[k], k * half, half)
            mine[...] = (
                mine[...].astype(jnp.float32) + far_in[g, k].astype(jnp.float32)
            ).astype(jnp.bfloat16)
            near_part(g, k, k).start()

    def stage_sum(g):
        h, l = place(g)
        mine = line(part, g, h)
        total = mine[...].astype(jnp.float32)
        arrived(near_in.at[g], near_recv.at[g])
        for k in range(2):
            total = total + near_in[g, k].astype(jnp.float32)
        mine[...] = total.astype(jnp.bfloat16)
        for k in range(3):
            light_part(g, k).start()

    def stage_return(g):
        h, l = place(g)
        total = one(part, g, h, l)[...].astype(jnp.float32)
        arrived(light_in.at[g], light_recv.at[g])
        for k in range(3):
            total = total + light_in[g, k].astype(jnp.float32)
        total = total.reshape(n_exp, PER, CAP, cols)
        back = jnp.stack([total[e] for e in range(n_exp)], axis=1).reshape(PER, chunk, cols)
        ret_out[g * PER : (g + 1) * PER] = back.astype(jnp.bfloat16)
        for p in range(g * PER, (g + 1) * PER):
            if p:
                give_back(p, mirror(p)).start()
            else:
                ret_in[0] = ret_out[0]


    stages = (
        stage_take,
        stage_spread,
        stage_pass,
        stage_compute,
        stage_join,
        stage_sum,
        stage_return,
    )
    pl.semaphore_wait(barrier, n_ep - 1 + 2 * (SIDE - 1))
    for p in range(1, n_ep):
        dispatch(p, mirror(p)).start()
    for step, (stage, g) in enumerate(PLAN):
        stages[stage](g)
        if step == COMBINE_AT:
            small[1].wait()
            weight = jnp.zeros((slots, n_tok), jnp.float32)
            for k in range(top):
                hit = rout_ref[k : k + 1, :] == slot_exp
                weight = weight + jnp.where(hit, gw_ref[k : k + 1, :], 0.0)
            combine[...] = (placing * weight).T

    both = combine[...]
    high = both.astype(jnp.bfloat16)
    low = (both - high.astype(jnp.float32)).astype(jnp.bfloat16)
    both = jnp.concatenate([high, low], axis=0)

    others = pl.ds(1, n_ep - 1)
    left(outgoing.at[others], disp_send)
    most = groups * len(steps) // SIDE
    left(rows.at[pl.ds(0, most), 0], a_send)
    left(rows.at[:, pl.ds(0, 2)], b_send)
    left(rows.at[:, 0], c_send)
    left(far_in, far_send)
    left(near_in, near_send)
    left(light_in, light_send)
    arrived(ret_in.at[others], ret_recv)
    back = ret_in[...].reshape(slots, cols)
    mixed = jnp.dot(both, back, preferred_element_type=jnp.float32)
    out_ref[...] = (mixed[:n_tok] + mixed[n_tok:]).astype(jnp.bfloat16)
    left(ret_out.at[others], ret_send)


def per_device(tokens, routing, gate_weights, norm_gain, w_gate, w_up, w_down):
    n_ep, n_tp = lax.axis_size("ep"), lax.axis_size("tp")
    n_exp, width, ff = w_gate.shape
    n_tok, cols = tokens.shape
    chunk = n_exp * CAP
    slots = n_ep * chunk
    groups, block = n_ep // PER, PER * chunk
    vmem = pl.BlockSpec(memory_space=pltpu.VMEM)
    hbm = pl.BlockSpec(memory_space=pltpu.HBM)
    bf16, f32 = jnp.bfloat16, jnp.float32
    dma = pltpu.SemaphoreType.DMA
    return pl.pallas_call(
        functools.partial(kernel, n_ep, n_tp),
        out_shape=jax.ShapeDtypeStruct((n_tok, cols), bf16),
        in_specs=[hbm] * 7,
        out_specs=vmem,
        scratch_shapes=[
            pltpu.VMEM(tokens.shape, bf16),
            pltpu.VMEM(routing.shape[::-1], jnp.int32),
            pltpu.VMEM(gate_weights.shape[::-1], f32),
            pltpu.VMEM((1, width), f32),
            pltpu.VMEM((n_exp, width, 2 * ff), bf16),
            pltpu.VMEM(w_down.shape, bf16),
            pltpu.VMEM((n_ep, chunk, cols), bf16),
            pltpu.VMEM((groups, SIDE, SIDE, block, cols), bf16),
            pltpu.VMEM((n_tok, slots), f32),
            pltpu.VMEM((groups, SIDE, SIDE, block, cols), bf16),
            pltpu.VMEM((groups, 2, SIDE // 2, block, cols), bf16),
            pltpu.VMEM((groups, 2, SIDE, block, cols), bf16),
            pltpu.VMEM((groups, 3, block, cols), bf16),
            pltpu.VMEM((n_ep, chunk, cols), bf16),
            pltpu.VMEM((n_ep, chunk, cols), bf16),
            dma((4,)),
            dma((3, n_exp)),
            dma,
            dma((groups,)),
            dma,
            dma((groups,)),
            dma,
            dma((groups, 2)),
            dma,
            dma((groups,)),
            dma,
            dma((groups,)),
            dma,
            dma((groups,)),
            dma,
            dma((groups,)),
            dma,
            dma,
        ],
        compiler_params=pltpu.CompilerParams(collective_id=0, has_side_effects=True),
    )(tokens, routing.T, gate_weights.T, norm_gain.reshape(1, width), w_gate, w_up, w_down)


def solution(mesh):
    in_specs = (
        P("ep", "tp"),
        P("ep", None),
        P("ep", None),
        P(),
        P("ep", None, "tp"),
        P("ep", None, "tp"),
        P("ep", "tp", None),
    )
    return jax.shard_map(
        per_device, mesh=mesh, in_specs=in_specs, out_specs=P("ep", "tp"), check_vma=False
    )
```
